32 devices in a mesh: grp: 1, sp: 8 (over z, core), tp: 4 (over y, x).
Axes of the slice: x: 2, y: 2, z: 4, core: 2. Of those that a mesh axis runs over, the one named last changes fastest.
Arguments:
- queries: bfloat16 [2048, 16, 128], P(('grp', 'sp'), 'tp'), may hold values from -6 to 6
- keys: bfloat16 [2048, 4, 128], P(('grp', 'sp'), 'tp'), may hold values from -6 to 6
- values: bfloat16 [2048, 4, 128], P(('grp', 'sp'), 'tp'), may hold values from -6 to 6
- log_gates: float32 [16, 2048], P('tp', ('grp', 'sp')), may hold values from -260 to 0, as said below
- documents: int32 [2048], P(('grp', 'sp')), may hold values from 0 to 2, never falling along the last dimension, each value on 1 to 1536 neighbouring positions
- query_gain: float32 [128], replicated, may hold values from 0.5 to 5
- key_gain: float32 [128], replicated, may hold values from 0.5 to 5
- out_weight: bfloat16 [2048, 2048], P('tp'), may hold values from -0.125 to 0.125
- residual: bfloat16 [2048, 2048], P(('grp', 'sp', 'tp')), may hold values from -1.5 to 1.5
- norm_gain: float32 [2048], replicated, may hold values from 0.1 to 1.9
- routes: int32 [2048, 2], P(('grp', 'sp', 'tp')), may hold values from 0 to 3, all different within a row; in each aligned block of 64 rows (0 to 63, 64 to 127, ...) at most 48 rows name the same one
- route_weights: float32 [2048, 2], P(('grp', 'sp', 'tp')), may hold values from 0.1 to 1
- w_gate: bfloat16 [8, 2048, 2048], P('sp', None, 'tp'), may hold values from -0.125 to 0.125
- w_up: bfloat16 [8, 2048, 2048], P('sp', None, 'tp'), may hold values from -0.125 to 0.125
- w_down: bfloat16 [8, 2048, 2048], P('sp', 'tp'), may hold values from -0.09375 to 0.09375
Outputs:
- layer_out: bfloat16 [2048, 2048], P(('grp', 'sp', 'tp'))
The draws below stay inside these ranges and needn't reach their ends.
Inputs may be any that keep to these rules, and one draw needn't show every extreme that they name: `log_gates`: non-increasing along positions for every head. `documents`: never falls along positions. `routes`: the 2 experts of a token differ; among the 64 tokens of one device (aligned blocks) no expert is named by more than 48 tokens, and in every draw some expert is named by exactly 48 of them.
All inputs are finite; a program needn't handle non-finite values.
Results may differ from the reference program's by a relative error of at most 0.017.
The reference program's roundings to bfloat16 on the way count: a program that leaves them out, or rounds other values in their place, can miss the bound.
Values may be sent and summed in bfloat16 or wider, within the bound.
A program may use at most 128 MiB of HBM per device.

```python
import math
import jax
import jax.numpy as jnp
import numpy as np
from jax import lax

QUERY_HEADS = 16
HEAD_DIM = 128
KV_HEADS = 4
D = 2048
FF_E = 4096
TOK_DEV = 256
DOCS = 3
TOP = 2
SEQUENCE_TOKENS = 2048
ROWS_DEV = 64
EXPERTS = 4
CAP = 48
N_TP = 4


def query_key_pair(key):
    base = jax.random.fold_in(key, 23)
    random_key_list = jax.random.split(base, 2)
    query_draw = jax.random.normal(random_key_list[0], (SEQUENCE_TOKENS, QUERY_HEADS, HEAD_DIM), jnp.float32)
    key_draw = jax.random.normal(random_key_list[1], (SEQUENCE_TOKENS, KV_HEADS, HEAD_DIM), jnp.float32)
    return (jnp.clip(query_draw, -6.0, 6.0), jnp.clip(key_draw, -6.0, 6.0))


def draw_queries(key, part):
    return query_key_pair(key)[0].astype(jnp.bfloat16)


def draw_keys(key, part):
    return query_key_pair(key)[1].astype(jnp.bfloat16)


def draw_values(key, part):
    random_key_list = jax.random.split(jax.random.fold_in(key, 31), 2)
    block_total = SEQUENCE_TOKENS // TOK_DEV
    offsets = jax.random.normal(random_key_list[0], (block_total, KV_HEADS, HEAD_DIM), jnp.float32)
    noise = jax.random.normal(random_key_list[1], (SEQUENCE_TOKENS, KV_HEADS, HEAD_DIM), jnp.float32)
    block_of = jnp.arange(SEQUENCE_TOKENS) // TOK_DEV
    drawn = offsets[block_of] + 0.7 * noise
    return jnp.clip(drawn, -6.0, 6.0).astype(jnp.bfloat16)


def gain_draw(key, salt):
    base = jax.random.fold_in(key, salt)
    return 1.0 + 0.18 * jnp.clip(jax.random.normal(base, (HEAD_DIM,), jnp.float32), -2.5, 2.5)


def draw_query_gain(key, part):
    return gain_draw(key, 41)


def draw_key_gain(key, part):
    return gain_draw(key, 43)


def draw_log_gates(key, part):
    random_key_list = jax.random.split(jax.random.fold_in(key, 11), 7)
    order = jax.random.permutation(random_key_list[0], QUERY_HEADS)
    slower_decay = order < QUERY_HEADS // 2
    fast_rate = jnp.exp(jax.random.uniform(random_key_list[1], (QUERY_HEADS,), jnp.float32, math.log(1.0 / 60.0), math.log(1.0 / 25.0)))
    slow_rate = jnp.exp(jax.random.uniform(random_key_list[2], (QUERY_HEADS,), jnp.float32, math.log(0.05), math.log(0.2))) / SEQUENCE_TOKENS
    rate = jnp.where(slower_decay, slow_rate, fast_rate)
    block_factor = jnp.exp(jax.random.uniform(random_key_list[3], (SEQUENCE_TOKENS // TOK_DEV,), jnp.float32, math.log(0.5), math.log(2.0)))
    token_position = jnp.arange(SEQUENCE_TOKENS)
    spread_factor = jax.random.uniform(random_key_list[4], (QUERY_HEADS, SEQUENCE_TOKENS), jnp.float32, 0.5, 1.5)
    logged_steps = -rate[:, None] * block_factor[token_position // TOK_DEV][None, :] * spread_factor
    surge_position = jax.random.randint(random_key_list[5], (2,), 0, SEQUENCE_TOKENS)
    surge_length = jnp.log(jax.random.uniform(random_key_list[6], (QUERY_HEADS, 2), jnp.float32, 0.5, 0.8))
    routing_hits = (token_position[None, :] == surge_position[:, None]).astype(jnp.float32)
    logged_steps = logged_steps + jnp.where(slower_decay[:, None], jnp.dot(surge_length, routing_hits), 0.0)
    return jnp.cumsum(logged_steps, axis=1)


def steps_of(stream_key, extent, pieces, least, largest):
    level, own = 1.0, jax.random.fold_in(stream_key, 6)
    for position, blocks in pieces:
        steps = jnp.exp(jax.random.uniform(jax.random.fold_in(own, position), (blocks,), jnp.float32, least / len(pieces), largest / len(pieces)))
        level = level * jnp.repeat(steps, extent[position] // blocks).reshape([-1 if axis == position else 1 for axis in range(len(extent))])
    return level


def profile(count, total, limit, slope):
    portions = [(1 << 20) // math.isqrt(grade ** slope) + 1 for grade in range(2, count + 1)]
    spare, holding = total - limit - (count - 1), [1] * (count - 1)
    while spare > 0:
        free = [i for i in range(count - 1) if holding[i] < limit]
        pool, remaining = sum([portions[i] for i in free]), spare
        for i in free:
            extra = min(limit - holding[i], max(1, remaining * portions[i] // pool), spare)
            holding[i] = holding[i] + extra
            spare = spare - extra
    return np.array([limit] + holding)


def uneven(rng, amount, total, limit, skew):
    if amount == 2:
        one = jax.random.randint(rng, (), max(1, total - limit), min(limit, total - 1) + 1)
        return jnp.stack([one, total - one])
    sizes = jnp.asarray(profile(amount, total, limit, skew), jnp.int32)
    twos = (amount - 1) // 2
    source_of, receiver = sizes[1:1 + 2 * twos:2], sizes[2:2 + 2 * twos:2]
    slack = jnp.minimum(source_of - 1, limit - receiver)
    passed = jax.random.randint(jax.random.fold_in(rng, 1), (twos,), 0, 1 << 20) % (slack + 1)
    sizes = sizes.at[1:1 + 2 * twos:2].set(source_of - passed).at[2:2 + 2 * twos:2].set(receiver + passed)
    return sizes[jax.random.permutation(jax.random.fold_in(rng, 2), amount)]


def assign_block(own_key, own, number, rows, number_of, top, bound, slope):
    sequence = jax.random.permutation(own_key, number_of)
    heavy_load, common = load_shares(number_of, rows * top, bound, slope, True), load_shares(number_of, rows * top, bound, slope, False)
    places = jnp.arange(number_of)

    def named(sizes, rotation):
        used = int((sizes > 0).sum())
        fixed = max(1, used // 4)
        shifted = fixed + (places - fixed + rotation * (used - fixed)) % max(1, number_of - fixed)
        return jnp.zeros((number_of,), jnp.int32).at[sequence[jnp.where(places < fixed, places, shifted)]].set(jnp.asarray(sizes, jnp.int32))

    sizes = jnp.where(number % 4 == 0, named(heavy_load, number // 4), named(common, number - number // 4 - 1))
    mixed = jax.random.permutation(jax.random.fold_in(own, 3), number_of)
    donor, receiver = mixed[0:number_of // 2 * 2:2], mixed[1:number_of // 2 * 2:2]
    room = jnp.minimum(sizes[donor] - 1, bound - sizes[receiver]) // 2
    room = jnp.where((donor == sequence[0]) | (receiver == sequence[0]) | (sizes[receiver] == 0), 0, jnp.maximum(room, 0))
    shifted = jax.random.randint(jax.random.fold_in(own, 4), (number_of // 2,), 0, 1 << 20) % (room + 1)
    sizes = sizes.at[donor].add(-shifted).at[receiver].add(shifted)
    items = jnp.searchsorted(jnp.cumsum(sizes), jnp.arange(rows * top), side="right").astype(jnp.int32)
    listing = items.reshape(top, rows).T
    listing = listing[jax.random.permutation(jax.random.fold_in(own, 1), rows)]
    rotation = jax.random.randint(jax.random.fold_in(own, 2), (rows, 1), 0, top)
    return jnp.take_along_axis(listing, (jnp.arange(top)[None, :] + rotation) % top, axis=1)


def load_shares(number_of, total, limit, lean, full):
    weights = [(1 << 20) // math.isqrt(rank ** lean) + 1 for rank in range(1, number_of + 1)]
    largest = limit if full else min(limit, max(-(-total // number_of), total * weights[0] // sum(weights)))
    least = 1 if total - largest >= number_of - 1 else 0
    holding, rest = [largest] + [least] * (number_of - 1), total - largest - least * (number_of - 1)
    while rest > 0:
        candidates = [i for i in range(1, number_of) if holding[i] < largest] or [i for i in range(1, number_of) if holding[i] < limit]
        whole, remaining = sum([weights[i] for i in candidates]), rest
        for i in candidates:
            more = min(limit - holding[i], max(1, remaining * weights[i] // whole), rest)
            holding[i] = holding[i] + more
            rest = rest - more
    return np.array(holding)


def scatter_about(key, dims, spread, most, cuts=(), held_as=jnp.bfloat16):
    level = steps_of(key, dims, cuts, -0.22, 0.18) if cuts else 1.0
    entries = jax.random.normal(key, dims, jnp.float32) * spread * level
    return jnp.minimum(jnp.maximum(entries, -most), most).astype(held_as)


def setup_inputs(seed: int = 0, part: int = 0) -> dict:
    streams_of = jax.random.split(jax.random.key(seed), 16)
    own_keys = jax.random.split(jax.random.fold_in(streams_of[15], part), 16)
    queries = draw_queries(jax.random.fold_in(jax.random.fold_in(streams_of[15], part), 71), part)
    keys = draw_keys(jax.random.fold_in(jax.random.fold_in(streams_of[15], part), 71), part)
    values = draw_values(jax.random.fold_in(jax.random.fold_in(streams_of[15], part), 71), part)
    log_gates = draw_log_gates(jax.random.fold_in(jax.random.fold_in(streams_of[15], part), 71), part)
    documents = jnp.searchsorted(jnp.cumsum(uneven(own_keys[4], DOCS, SEQUENCE_TOKENS, 3 * SEQUENCE_TOKENS // 4, 0)), jnp.arange(SEQUENCE_TOKENS), side="right").astype(jnp.int32)
    query_gain = draw_query_gain(jax.random.fold_in(streams_of[15], 71), part)
    key_gain = draw_key_gain(jax.random.fold_in(streams_of[15], 71), part)
    out_weight = scatter_about(streams_of[7], (D, D), D ** -0.5, 0.125, ((0, 4),))
    residual = scatter_about(own_keys[8], (SEQUENCE_TOKENS, D), 0.25, 1.5, ((0, 32),))
    norm_gain = jnp.clip(1.0 + 0.18 * jax.random.normal(streams_of[9], (D,), jnp.float32), 0.1, 1.9)
    routes_keys = jax.random.split(jax.random.fold_in(own_keys[10], 1), SEQUENCE_TOKENS // ROWS_DEV)
    routes_turns = jax.random.permutation(jax.random.fold_in(own_keys[10], 3), SEQUENCE_TOKENS // ROWS_DEV)
    routes = jax.vmap(lambda own, number: assign_block(jax.random.fold_in(own_keys[10], 2), own, number, ROWS_DEV, EXPERTS, TOP, CAP, 2))(routes_keys, routes_turns).reshape((SEQUENCE_TOKENS, TOP))
    route_weights = jnp.clip(0.1 + 0.9 * jax.random.uniform(own_keys[11], (SEQUENCE_TOKENS, TOP), jnp.float32) ** steps_of(own_keys[11], (SEQUENCE_TOKENS, TOP), ((0, 32),), -0.2, 0.2), 0.1, 1.0)
    w_gate = scatter_about(streams_of[12], (2 * EXPERTS, D, FF_E // 2), D ** -0.5, 0.125, ((0, 8), (2, 4)))
    w_up = scatter_about(streams_of[13], (2 * EXPERTS, D, FF_E // 2), D ** -0.5, 0.125, ((0, 8), (2, 4)))
    w_down = scatter_about(streams_of[14], (2 * EXPERTS, FF_E // 2, D), FF_E ** -0.5, 0.09375, ((0, 8), (1, 4)))
    return dict(queries=queries, keys=keys, values=values, log_gates=log_gates, documents=documents, query_gain=query_gain, key_gain=key_gain, out_weight=out_weight, residual=residual, norm_gain=norm_gain, routes=routes, route_weights=route_weights, w_gate=w_gate, w_up=w_up, w_down=w_down)


EPSILON = 1e-06

def rms_scale(inputs, gain):
    return inputs * lax.rsqrt(lax.optimization_barrier(jnp.mean(inputs * inputs, axis=-1, keepdims=True)) + EPSILON) * gain

def round_trip(array):
    return lax.optimization_barrier(array.astype(jnp.bfloat16)).astype(jnp.float32)

def reference(queries, keys, values, log_gates, documents, query_gain, key_gain, out_weight, residual, norm_gain, routes, route_weights, w_gate, w_up, w_down):
    total_len, head_count, head_size = queries.shape
    kv_count = keys.shape[1]
    group_size = head_count // kv_count
    model_dim = residual.shape[1]
    query_norm = round_trip(rms_scale(queries.astype(jnp.float32), query_gain) * head_size ** (-0.5))
    key_norm = round_trip(rms_scale(keys.astype(jnp.float32), key_gain))
    value_full = values.astype(jnp.float32)
    key_pos = jnp.arange(total_len, dtype=jnp.int32)
    block_rows = 256

    def attend_block(block_index):
        start = block_index * block_rows
        query_block = lax.dynamic_slice_in_dim(query_norm, start, block_rows, 0).reshape(block_rows, kv_count, group_size, head_size)
        scores = jnp.einsum('bkgd,skd->kgbs', query_block, key_norm, precision=lax.Precision.HIGHEST)
        scores = scores.reshape(head_count, block_rows, total_len)
        query_gates = lax.dynamic_slice_in_dim(log_gates, start, block_rows, 1)
        scores = scores + query_gates[:, :, None] - log_gates[:, None, :]
        query_pos = start + jnp.arange(block_rows, dtype=jnp.int32)
        query_docs = lax.dynamic_slice_in_dim(documents, start, block_rows, 0)
        allowed = (key_pos[None, :] <= query_pos[:, None]) & (documents[None, :] == query_docs[:, None])
        scores = jnp.where(allowed[None], scores, -jnp.inf)
        peak = lax.optimization_barrier(jnp.max(scores, axis=-1, keepdims=True))
        expo = jnp.exp(scores - peak)
        denom = lax.optimization_barrier(jnp.sum(expo, axis=-1))
        weights = round_trip(expo).reshape(kv_count, group_size, block_rows, total_len)
        mixed_heads = jnp.einsum('kgbs,skd->bkgd', weights, value_full, precision=lax.Precision.HIGHEST)
        denom_rows = jnp.transpose(denom.reshape(kv_count, group_size, block_rows), (2, 0, 1))
        return (mixed_heads / denom_rows[..., None]).astype(jnp.bfloat16).reshape(block_rows, model_dim)
    attended = lax.map(attend_block, jnp.arange(total_len // block_rows, dtype=jnp.int32)).reshape(total_len, model_dim)
    projected = jnp.dot(attended, out_weight, preferred_element_type=jnp.float32)
    mixed = (residual.astype(jnp.float32) + projected).astype(jnp.bfloat16)
    normed = rms_scale(mixed.astype(jnp.float32), norm_gain).astype(jnp.bfloat16)
    rows_dev = TOK_DEV // N_TP
    block_count = total_len // rows_dev
    slot_count = block_count * CAP
    quarter = FF_E // (2 * N_TP)
    token_ids = jnp.arange(total_len, dtype=jnp.int32)

    def one_expert(summed, expert_index):
        chosen = routes == expert_index
        picked = jnp.any(chosen, axis=1)
        weight = lax.optimization_barrier(jnp.sum(jnp.where(chosen, route_weights, 0.0), axis=1))
        counts = picked.astype(jnp.int32).reshape(block_count, rows_dev)
        rank = (jnp.cumsum(counts, axis=1) - 1).reshape(total_len)
        slot = token_ids // rows_dev * CAP + rank
        slot = jnp.where(picked, slot, slot_count).astype(jnp.int32)
        owner = jnp.zeros((slot_count + 1,), jnp.int32).at[slot].set(token_ids)[:slot_count]
        slot_weight = jnp.zeros((slot_count + 1,), jnp.float32).at[slot].set(weight)[:slot_count]
        rows_in = normed[owner]
        expert_sum = jnp.zeros((slot_count, model_dim), jnp.float32)
        for half in range(2):
            entry = (2 * expert_index + half).astype(jnp.int32)
            gate_all = lax.dynamic_index_in_dim(w_gate, entry, 0, keepdims=False)
            up_all = lax.dynamic_index_in_dim(w_up, entry, 0, keepdims=False)
            down_all = lax.dynamic_index_in_dim(w_down, entry, 0, keepdims=False)
            for column in range(N_TP):
                lower = column * quarter
                gate_act = jnp.dot(rows_in, gate_all[:, lower:lower + quarter], preferred_element_type=jnp.float32)
                up_act = jnp.dot(rows_in, up_all[:, lower:lower + quarter], preferred_element_type=jnp.float32)
                hidden = (jax.nn.silu(gate_act) * up_act).astype(jnp.bfloat16)
                partial_out = jnp.dot(hidden, down_all[lower:lower + quarter, :], preferred_element_type=jnp.float32)
                expert_sum = expert_sum + round_trip(partial_out)
        summed = summed.at[owner].add(slot_weight[:, None] * expert_sum)
        return (summed, None)
    start_sum = jnp.zeros((total_len, model_dim), jnp.float32)
    routed, _ = lax.scan(one_expert, start_sum, jnp.arange(EXPERTS, dtype=jnp.int32))
    return (mixed.astype(jnp.float32) + routed).astype(jnp.bfloat16)
```

```python
import functools

import jax
import jax.numpy as jnp
from jax import lax
from jax.experimental import pallas as pl
from jax.experimental.pallas import tpu as pltpu
from jax.sharding import PartitionSpec as P

EPSILON = 1e-06
CHUNK = 16
MESH = pl.DeviceIdType.MESH


def rms_scale(inputs, gain):
    return inputs * lax.rsqrt(jnp.mean(inputs * inputs, axis=-1, keepdims=True) + EPSILON) * gain


def flip(index, bits):
    index = index + (bits % 2) * (1 - 2 * (index % 2))
    return index + (bits // 2) * (2 - 4 * ((index // 2) % 2))


def greet(nz, n_tp, z, c, t):
    barrier = pltpu.get_barrier_semaphore()
    for dz in range(1, nz):
        pl.semaphore_signal(
            barrier, inc=1, device_id={"sp": 2 * ((z + dz) % nz) + c}, device_id_type=MESH
        )
    for k in range(1, n_tp):
        pl.semaphore_signal(barrier, inc=1, device_id={"tp": flip(t, k)}, device_id_type=MESH)
    pl.semaphore_signal(barrier, inc=1, device_id={"sp": 2 * z + 1 - c}, device_id_type=MESH)
    pl.semaphore_wait(barrier, nz - 1 + n_tp - 1 + 1)


def attend_kernel(
    nz,
    n_tp,
    q_ref,
    kv_ref,
    gd_ref,
    col_ref,
    w_ref,
    res_ref,
    gain_ref,
    mixed_ref,
    normed_ref,
    kv_buf,
    gd_buf,
    m_ref,
    l_ref,
    acc_ref,
    att_ref,
    sbuf,
    rbuf,
    kv_send,
    kv_recv,
    gd_send,
    gd_recv,
    fkv_send,
    fgd_send,
    rs_send,
    rs_recv,
):
    s = lax.axis_index("sp")
    t = lax.axis_index("tp")
    z, c = s // 2, s % 2
    heads, rows, hd = q_ref.shape
    greet(nz, n_tp, z, c, t)

    def own_copies(slot, target):
        return (
            pltpu.make_async_remote_copy(
                kv_ref, kv_buf.at[s], kv_send.at[slot], kv_recv.at[s],
                device_id={"sp": target}, device_id_type=MESH,
            ),
            pltpu.make_async_remote_copy(
                gd_ref, gd_buf.at[s], gd_send.at[slot], gd_recv.at[s],
                device_id={"sp": target}, device_id_type=MESH,
            ),
        )

    def fwd_copies(source, slot):
        return (
            pltpu.make_async_remote_copy(
                kv_buf.at[source], kv_buf.at[source], fkv_send.at[slot], kv_recv.at[source],
                device_id={"sp": 2 * z + 1 - c}, device_id_type=MESH,
            ),
            pltpu.make_async_remote_copy(
                gd_buf.at[source], gd_buf.at[source], fgd_send.at[slot], gd_recv.at[source],
                device_id={"sp": 2 * z + 1 - c}, device_id_type=MESH,
            ),
        )

    def begin(dz, carry):
        for copy in own_copies(dz, 2 * (z + dz) + c):
            copy.start()
        return carry

    @pl.when(c == 0)
    def _():
        for copy in own_copies(0, 2 * z + 1):
            copy.start()

    lax.fori_loop(1, nz - z, begin, 0)

    def update(keys, values, gates, docs, causal, first):
        same = docs == col_ref[:, heads:heads + 1]
        if causal:
            qi = lax.broadcasted_iota(jnp.int32, (rows, rows), 0)
            ki = lax.broadcasted_iota(jnp.int32, (rows, rows), 1)
            same = same & (ki <= qi)
        for h in range(heads):
            scores = lax.dot_general(
                q_ref[h], keys, (((1,), (1,)), ((), ())), preferred_element_type=jnp.float32
            )
            scores = scores + col_ref[:, h:h + 1] - gates[h:h + 1, :]
            scores = jnp.where(same, scores, -jnp.inf)
            peak = jnp.max(scores, axis=-1, keepdims=True)
            if first:
                expo = jnp.exp(scores - peak)
                l_ref[h] = jnp.sum(expo, axis=-1, keepdims=True)
                m_ref[h] = peak
                acc_ref[h] = jnp.dot(
                    expo.astype(jnp.bfloat16), values, preferred_element_type=jnp.float32
                )
            else:
                old = m_ref[h]
                new = jnp.maximum(old, peak)
                expo = jnp.exp(scores - new)
                factor = jnp.exp(old - new)
                l_ref[h] = factor * l_ref[h] + jnp.sum(expo, axis=-1, keepdims=True)
                m_ref[h] = new
                acc_ref[h] = factor * acc_ref[h] + jnp.dot(
                    expo.astype(jnp.bfloat16), values, preferred_element_type=jnp.float32
                )

    update(
        kv_ref[:, :hd], kv_ref[:, hd:], gd_ref[...], gd_ref[heads:heads + 1, :], True, True
    )

    def take(source):
        update(
            kv_buf[source, :, :hd],
            kv_buf[source, :, hd:],
            gd_buf[source],
            gd_buf[source, heads:heads + 1, :],
            False,
            False,
        )

    def one_source(i, carry):
        dz = (i + 1) // 2
        direct = i % 2
        core = (1 - direct) * (1 - c) + direct * c
        source = 2 * (z - dz) + core
        for copy in fwd_copies(source, dz):
            copy.wait_recv()

        @pl.when(direct == 1)
        def _():
            for copy in fwd_copies(source, dz):
                copy.start()

        take(source)
        return carry

    lax.fori_loop(1 - c, 2 * z + 1, one_source, 0)

    for h in range(heads):
        att_ref[:, h * hd:(h + 1) * hd] = (acc_ref[h] / l_ref[h]).astype(jnp.bfloat16)

    share = rows // n_tp

    def project(i, carry):
        k = n_tp - 1 - i
        start = pl.multiple_of(flip(t, k) * share, share)
        block = jnp.dot(
            att_ref[pl.ds(start, share), :], w_ref[...], preferred_element_type=jnp.float32
        )
        sbuf[k] = block.astype(jnp.bfloat16)

        @pl.when(k > 0)
        def _():
            pltpu.make_async_remote_copy(
                sbuf.at[k], rbuf.at[k], rs_send.at[k], rs_recv.at[k],
                device_id={"tp": flip(t, k)}, device_id_type=MESH,
            ).start()

        return carry

    lax.fori_loop(0, n_tp, project, 0)

    for k in range(1, n_tp):
        copy = pltpu.make_async_remote_copy(
            sbuf.at[k], rbuf.at[k], rs_send.at[k], rs_recv.at[k],
            device_id={"tp": flip(t, k)}, device_id_type=MESH,
        )
        copy.wait_recv()

    def finish(i, carry):
        part = pl.ds(pl.multiple_of(i * CHUNK, CHUNK), CHUNK)
        total = sbuf[0, part, :].astype(jnp.float32)
        for k in range(1, n_tp):
            total = total + rbuf[k, part, :].astype(jnp.float32)
        mixed = (res_ref[part, :].astype(jnp.float32) + total).astype(jnp.bfloat16)
        mixed_ref[part, :] = mixed
        normed_ref[part, :] = rms_scale(mixed.astype(jnp.float32), gain_ref[...]).astype(
            jnp.bfloat16
        )
        return carry

    lax.fori_loop(0, share // CHUNK, finish, 0)

    for k in range(1, n_tp):
        pltpu.make_async_remote_copy(
            sbuf.at[k], rbuf.at[k], rs_send.at[k], rs_recv.at[k],
            device_id={"tp": flip(t, k)}, device_id_type=MESH,
        ).wait_send()

    def end(dz, carry):
        for copy in own_copies(dz, 2 * (z + dz) + c):
            copy.wait_send()
        return carry

    @pl.when(c == 0)
    def _():
        for copy in own_copies(0, 2 * z + 1):
            copy.wait_send()

    lax.fori_loop(1, nz - z, end, 0)

    def end_forward(dz, carry):
        for copy in fwd_copies(2 * (z - dz) + c, dz):
            copy.wait_send()
        return carry

    lax.fori_loop(1, z + 1, end_forward, 0)


def expert_kernel(
    nz,
    n_tp,
    out_ref,
    wg_hbm,
    wu_hbm,
    wd_hbm,
    ret_ref,
    wg_ref,
    wu_ref,
    wd_ref,
    arrived,
    part,
    pbuf,
    rbuf,
    hbuf,
    fin,
    w_sem,
    a_send,
    a_recv,
    b_send,
    b_recv,
    f_send,
    f_recv,
    d_send,
    d_recv,
    p_send,
    p_recv,
    h_send,
    h_recv,
    r_send,
    r_recv,
    z_send,
    z_recv,
):
    s = lax.axis_index("sp")
    t = lax.axis_index("tp")
    z, c = s // 2, s % 2
    _, cap, width = out_ref.shape
    rows = nz * cap
    half = nz // 2
    partner = {"sp": 2 * z + 1 - c}

    loads = [
        pltpu.make_async_copy(src, dst, w_sem.at[i])
        for i, (src, dst) in enumerate(((wg_hbm, wg_ref), (wu_hbm, wu_ref), (wd_hbm, wd_ref)))
    ]
    for load in loads:
        load.start()
    greet(nz, n_tp, z, c, t)

    def remote(src, dst, send, recv, where):
        return pltpu.make_async_remote_copy(
            src, dst, send, recv, device_id=where, device_id_type=MESH
        )

    mine = 2 * t + c

    def along(dz):
        target = (z + dz) % nz
        return remote(
            out_ref.at[target], arrived.at[mine, z], a_send.at[dz], a_recv.at[dz],
            {"sp": 2 * target + c},
        )

    def spread(dz, k, src):
        zs = (z + nz - dz) % nz
        return remote(
            src, arrived.at[mine, zs], b_send.at[k, zs], b_recv.at[k, zs], {"tp": flip(t, k)}
        )

    def share_own(dz, src):
        zs = (z + nz - dz) % nz
        return remote(src, arrived.at[mine, zs], b_send.at[0, zs], b_recv.at[0, zs], partner)

    def begin(dz, carry):
        along(dz).start()
        return carry

    for k in (1, 2):
        spread(0, k, out_ref.at[z]).start()
    share_own(0, out_ref.at[z]).start()
    lax.fori_loop(1, nz, begin, 0)
    arrived[mine, z] = out_ref[z]

    def pass_on(dz, carry):
        zs = (z + nz - dz) % nz
        remote(
            out_ref.at[zs], arrived.at[mine, zs], a_send.at[dz], a_recv.at[dz], partner
        ).wait_recv()
        for k in (1, 2):
            spread(dz, k, arrived.at[mine, zs]).start()
        share_own(dz, arrived.at[mine, zs]).start()
        return carry

    lax.fori_loop(1, nz, pass_on, 0)

    def b_wait(k):
        source = 2 * flip(t, k) + c if k else 2 * t + 1 - c

        def one(zs, carry):
            remote(
                arrived.at[source, zs], arrived.at[source, zs], b_send.at[k, zs],
                b_recv.at[k, zs], partner,
            ).wait_recv()
            return carry

        lax.fori_loop(0, nz, one, 0)

    def diagonal(k):
        source = 2 * flip(t, 3 - k) + c
        blocks = pl.ds(0, half) if k == 1 else pl.ds(half, nz - half)
        where = arrived.at[source, blocks]
        return remote(where, where, f_send.at[k], f_recv.at[k], {"tp": flip(t, k)})

    def diagonal_in(k):
        source = 2 * flip(t, 3) + c
        blocks = pl.ds(0, half) if k == 1 else pl.ds(half, nz - half)
        where = arrived.at[source, blocks]
        return remote(where, where, f_send.at[k], f_recv.at[k], {"tp": flip(t, k)})

    def to_partner(k):
        group = arrived.at[2 * flip(t, k) + c]
        return remote(group, group, d_send.at[k], d_recv.at[k], partner)

    def from_partner(k):
        group = arrived.at[2 * flip(t, k) + 1 - c]
        return remote(group, group, d_send.at[k], d_recv.at[k], partner)

    def part_out(k):
        return remote(part.at[1, k], pbuf.at[k], p_send.at[k], p_recv.at[k], partner)

    low, high = pl.ds(0, half), pl.ds(half, nz - half)

    def reduce_out(k, piece):
        blocks = high if piece else low
        return remote(
            part.at[0, k, blocks], rbuf.at[k, blocks], r_send.at[k, piece], r_recv.at[k, piece],
            {"tp": flip(t, k)},
        )

    def hand_over(k):
        blocks = low if k == 1 else high
        return remote(
            part.at[0, 3, blocks], hbuf.at[blocks], h_send.at[k], h_recv.at[k],
            {"tp": flip(t, k)},
        )

    def add_pair(k):
        def one(i, carry):
            b, r = i // (cap // CHUNK), i % (cap // CHUNK)
            at = pl.ds(pl.multiple_of(r * CHUNK, CHUNK), CHUNK)
            total = part[0, k, b, at, :].astype(jnp.float32) + pbuf[k, b, at, :].astype(
                jnp.float32
            )
            part[0, k, b, at, :] = total.astype(jnp.bfloat16)
            return carry

        part_out(k).wait_recv()
        lax.fori_loop(0, rows // CHUNK, one, 0)

    def add_handed(k, first, count):
        def one(i, carry):
            b, r = first + i // (cap // CHUNK), i % (cap // CHUNK)
            at = pl.ds(pl.multiple_of(r * CHUNK, CHUNK), CHUNK)
            total = part[0, k, b, at, :].astype(jnp.float32) + hbuf[b, at, :].astype(jnp.float32)
            part[0, k, b, at, :] = total.astype(jnp.bfloat16)
            return carry

        lax.fori_loop(0, count * (cap // CHUNK), one, 0)

    for load in loads:
        load.wait()

    def compute(i, carry):
        k, other = i // 2, i % 2

        @pl.when(i == 1)
        def _():
            b_wait(0)

        @pl.when(i == 2)
        def _():
            b_wait(1)
            diagonal(2).start()
            to_partner(1).start()
            b_wait(2)
            diagonal(1).start()
            to_partner(2).start()
            add_pair(0)

        @pl.when(i == 3)
        def _():
            from_partner(1).wait_recv()

        @pl.when(i == 4)
        def _():
            add_pair(1)
            reduce_out(1, 0).start()

        @pl.when(i == 5)
        def _():
            from_partner(2).wait_recv()

        @pl.when(i == 6)
        def _():
            add_pair(2)
            reduce_out(2, 1).start()
            diagonal_in(1).wait_recv()
            diagonal_in(2).wait_recv()
            to_partner(3).start()

        @pl.when(i == 7)
        def _():
            from_partner(3).wait_recv()

        column = 2 * flip(t, k) + other * (1 - c) + (1 - other) * c
        flat = arrived[column].reshape(rows, width)
        gate = jnp.dot(flat, wg_ref[...], preferred_element_type=jnp.float32)
        up = jnp.dot(flat, wu_ref[...], preferred_element_type=jnp.float32)
        hidden = (gate * (1.0 / (1.0 + jnp.exp(-gate))) * up).astype(jnp.bfloat16)
        result = jnp.dot(hidden, wd_ref[...], preferred_element_type=jnp.float32)
        part[other, k] = result.astype(jnp.bfloat16).reshape(nz, cap, width)

        for kk in range(n_tp):
            @pl.when(i == 2 * kk + 1)
            def _():
                part_out(kk).start()

        return carry

    lax.fori_loop(0, 2 * n_tp, compute, 0)

    add_pair(3)
    hand_over(1).start()
    hand_over(2).start()
    hand_over(1).wait_recv()
    add_handed(2, 0, half)
    reduce_out(2, 0).start()
    hand_over(2).wait_recv()
    add_handed(1, half, nz - half)
    reduce_out(1, 1).start()

    def home(dz):
        target = (z + dz) % nz
        return remote(
            fin.at[target], ret_ref.at[z], z_send.at[dz], z_recv.at[dz], {"sp": 2 * target + c}
        )

    def total_block(zs, dst, index):
        for r in range(cap // CHUNK):
            at = pl.ds(r * CHUNK, CHUNK)
            total = (
                part[0, 0, zs, at, :].astype(jnp.float32)
                + rbuf[1, zs, at, :].astype(jnp.float32)
                + rbuf[2, zs, at, :].astype(jnp.float32)
            )
            dst[index, at, :] = total.astype(jnp.bfloat16)

    for k in (1, 2):
        for piece in (0, 1):
            reduce_out(k, piece).wait_recv()

    def send_home(i, carry):
        dz = nz - 1 - i
        target = (z + dz) % nz
        total_block(target, fin, target)
        home(dz).start()
        return carry

    lax.fori_loop(0, nz - 1, send_home, 0)
    total_block(z, ret_ref, z)

    def collect(dz, carry):
        zs = (z + nz - dz) % nz
        remote(
            fin.at[zs], ret_ref.at[zs], z_send.at[dz], z_recv.at[dz], partner
        ).wait_recv()
        return carry

    lax.fori_loop(1, nz, collect, 0)

    def drain(dz, carry):
        along(dz).wait_send()
        home(dz).wait_send()
        return carry

    lax.fori_loop(1, nz, drain, 0)

    def drain_spread(dz, carry):
        for k in (1, 2):
            spread(dz, k, out_ref.at[z]).wait_send()
        share_own(dz, out_ref.at[z]).wait_send()
        return carry

    lax.fori_loop(0, nz, drain_spread, 0)
    for k in (1, 2):
        diagonal(k).wait_send()
        hand_over(k).wait_send()
        for piece in (0, 1):
            reduce_out(k, piece).wait_send()
    for k in range(1, n_tp):
        to_partner(k).wait_send()
    for k in range(n_tp):
        part_out(k).wait_send()


def local(
    nz,
    n_tp,
    queries,
    keys,
    values,
    log_gates,
    documents,
    query_gain,
    key_gain,
    out_weight,
    residual,
    norm_gain,
    routes,
    route_weights,
    w_gate,
    w_up,
    w_down,
):
    tok_dev, heads, head_size = queries.shape
    model_dim = residual.shape[1]
    rows_dev = tok_dev // n_tp
    n_sp = 2 * nz
    query_norm = (rms_scale(queries.astype(jnp.float32), query_gain) * head_size ** (-0.5)).astype(
        jnp.bfloat16
    )
    key_norm = rms_scale(keys[:, 0, :].astype(jnp.float32), key_gain).astype(jnp.bfloat16)
    kv = jnp.concatenate([key_norm, values[:, 0, :]], axis=1)
    pad = (-(heads + 1)) % 8
    gates_docs = jnp.concatenate(
        [
            log_gates,
            documents.astype(jnp.float32)[None, :],
            jnp.zeros((pad, tok_dev), jnp.float32),
        ],
        axis=0,
    )
    vmem = pl.BlockSpec(memory_space=pltpu.VMEM)
    hbm = pl.BlockSpec(memory_space=pl.ANY)
    dma = pltpu.SemaphoreType.DMA
    mixed, normed = pl.pallas_call(
        functools.partial(attend_kernel, nz, n_tp),
        out_shape=(
            jax.ShapeDtypeStruct((rows_dev, model_dim), jnp.bfloat16),
            jax.ShapeDtypeStruct((rows_dev, model_dim), jnp.bfloat16),
        ),
        in_specs=[vmem] * 7,
        out_specs=(vmem, vmem),
        scratch_shapes=[
            pltpu.VMEM((n_sp,) + kv.shape, jnp.bfloat16),
            pltpu.VMEM((n_sp,) + gates_docs.shape, jnp.float32),
            pltpu.VMEM((heads, tok_dev, 1), jnp.float32),
            pltpu.VMEM((heads, tok_dev, 1), jnp.float32),
            pltpu.VMEM((heads, tok_dev, head_size), jnp.float32),
            pltpu.VMEM((tok_dev, heads * head_size), jnp.bfloat16),
            pltpu.VMEM((n_tp, rows_dev, model_dim), jnp.bfloat16),
            pltpu.VMEM((n_tp, rows_dev, model_dim), jnp.bfloat16),
            dma((nz,)),
            dma((n_sp,)),
            dma((nz,)),
            dma((n_sp,)),
            dma((nz,)),
            dma((nz,)),
            dma((n_tp,)),
            dma((n_tp,)),
        ],
        compiler_params=pltpu.CompilerParams(
            collective_id=0, has_side_effects=True, vmem_limit_bytes=56 * 1024 * 1024
        ),
        name="attend",
    )(
        jnp.transpose(query_norm, (1, 0, 2)),
        kv,
        gates_docs,
        gates_docs.T,
        out_weight,
        residual,
        norm_gain[None, :],
    )

    experts = nz
    named = min(rows_dev, 6 * rows_dev // n_sp)
    capacity = named + (-named) % CHUNK
    expert_ids = jnp.arange(experts, dtype=jnp.int32)
    chosen = routes[:, :, None] == expert_ids[None, None, :]
    picked = jnp.sum(chosen.astype(jnp.float32), axis=1)
    weight_of = jnp.sum(jnp.where(chosen, route_weights[:, :, None], 0.0), axis=1)
    rank = jnp.cumsum(picked, axis=0) - 1.0
    slot_ids = jnp.arange(capacity).astype(jnp.float32)
    placing = picked.T[:, None, :] * (rank.T[:, None, :] == slot_ids[None, :, None]).astype(
        jnp.float32
    )
    outgoing = jnp.einsum(
        "ecr,rd->ecd", placing.astype(jnp.bfloat16), normed, preferred_element_type=jnp.float32
    ).astype(jnp.bfloat16)

    hidden_dev = w_gate.shape[2]
    block = (nz, capacity, model_dim)
    returned = pl.pallas_call(
        functools.partial(expert_kernel, nz, n_tp),
        out_shape=jax.ShapeDtypeStruct(block, jnp.bfloat16),
        in_specs=[vmem, hbm, hbm, hbm],
        out_specs=vmem,
        scratch_shapes=[
            pltpu.VMEM((model_dim, hidden_dev), jnp.bfloat16),
            pltpu.VMEM((model_dim, hidden_dev), jnp.bfloat16),
            pltpu.VMEM((hidden_dev, model_dim), jnp.bfloat16),
            pltpu.VMEM((2 * n_tp,) + block, jnp.bfloat16),
            pltpu.VMEM((2, n_tp) + block, jnp.bfloat16),
            pltpu.VMEM((n_tp,) + block, jnp.bfloat16),
            pltpu.VMEM((3,) + block, jnp.bfloat16),
            pltpu.VMEM(block, jnp.bfloat16),
            pltpu.VMEM(block, jnp.bfloat16),
            dma((3,)),
            dma((nz,)),
            dma((nz,)),
            dma((3, nz)),
            dma((3, nz)),
            dma((3,)),
            dma((3,)),
            dma((n_tp,)),
            dma((n_tp,)),
            dma((n_tp,)),
            dma((n_tp,)),
            dma((3,)),
            dma((3,)),
            dma((3, 2)),
            dma((3, 2)),
            dma((nz,)),
            dma((nz,)),
        ],
        compiler_params=pltpu.CompilerParams(
            collective_id=1, has_side_effects=True, vmem_limit_bytes=60 * 1024 * 1024
        ),
        name="experts",
    )(outgoing, w_gate[0], w_up[0], w_down[0])

    combining = placing * weight_of.T[:, None, :]
    routed = jnp.einsum(
        "ecr,ecd->rd", combining, returned.astype(jnp.float32), precision=lax.Precision.HIGHEST
    )
    return (mixed.astype(jnp.float32) + routed).astype(jnp.bfloat16)


def solution(mesh):
    return jax.shard_map(
        functools.partial(local, mesh.shape["sp"] // 2, mesh.shape["tp"]),
        mesh=mesh,
        in_specs=(
            P(("grp", "sp"), "tp", None),
            P(("grp", "sp"), "tp", None),
            P(("grp", "sp"), "tp", None),
            P("tp", ("grp", "sp")),
            P(("grp", "sp")),
            P(),
            P(),
            P("tp", None),
            P(("grp", "sp", "tp"), None),
            P(),
            P(("grp", "sp", "tp"), None),
            P(("grp", "sp", "tp"), None),
            P("sp", None, "tp"),
            P("sp", None, "tp"),
            P("sp", "tp", None),
        ),
        out_specs=P(("grp", "sp", "tp"), None),
        check_vma=False,
    )
```

```python
import functools

import jax
import jax.numpy as jnp
from jax import lax
from jax.experimental import pallas as pl
from jax.experimental.pallas import tpu as pltpu
from jax.sharding import PartitionSpec as P

EPSILON = 1e-06
CHUNK = 16
MESH = pl.DeviceIdType.MESH


def rms_scale(inputs, gain):
    return inputs * lax.rsqrt(jnp.mean(inputs * inputs, axis=-1, keepdims=True) + EPSILON) * gain


def flip(index, bits):
    index = index + (bits % 2) * (1 - 2 * (index % 2))
    return index + (bits // 2) * (2 - 4 * ((index // 2) % 2))


def greet(nz, n_tp, z, c, t):
    barrier = pltpu.get_barrier_semaphore()
    for dz in range(1, nz):
        pl.semaphore_signal(
            barrier, inc=1, device_id={"sp": 2 * ((z + dz) % nz) + c}, device_id_type=MESH
        )
    for k in range(1, n_tp):
        pl.semaphore_signal(barrier, inc=1, device_id={"tp": flip(t, k)}, device_id_type=MESH)
    pl.semaphore_signal(barrier, inc=1, device_id={"sp": 2 * z + 1 - c}, device_id_type=MESH)
    pl.semaphore_wait(barrier, nz - 1 + n_tp - 1 + 1)


def attend_kernel(
    nz,
    n_tp,
    q_ref,
    kv_ref,
    gd_ref,
    col_ref,
    w_ref,
    res_ref,
    gain_ref,
    mixed_ref,
    normed_ref,
    kv_buf,
    gd_buf,
    m_ref,
    l_ref,
    acc_ref,
    att_ref,
    sbuf,
    rbuf,
    kv_send,
    kv_recv,
    gd_send,
    gd_recv,
    fkv_send,
    fgd_send,
    rs_send,
    rs_recv,
):
    s = lax.axis_index("sp")
    t = lax.axis_index("tp")
    z, c = s // 2, s % 2
    heads, rows, hd = q_ref.shape
    greet(nz, n_tp, z, c, t)

    def own_copies(slot, target):
        return (
            pltpu.make_async_remote_copy(
                kv_ref, kv_buf.at[s], kv_send.at[slot], kv_recv.at[s],
                device_id={"sp": target}, device_id_type=MESH,
            ),
            pltpu.make_async_remote_copy(
                gd_ref, gd_buf.at[s], gd_send.at[slot], gd_recv.at[s],
                device_id={"sp": target}, device_id_type=MESH,
            ),
        )

    def fwd_copies(source, slot):
        return (
            pltpu.make_async_remote_copy(
                kv_buf.at[source], kv_buf.at[source], fkv_send.at[slot], kv_recv.at[source],
                device_id={"sp": 2 * z + 1 - c}, device_id_type=MESH,
            ),
            pltpu.make_async_remote_copy(
                gd_buf.at[source], gd_buf.at[source], fgd_send.at[slot], gd_recv.at[source],
                device_id={"sp": 2 * z + 1 - c}, device_id_type=MESH,
            ),
        )

    def begin(dz, carry):
        for copy in own_copies(dz, 2 * (z + dz) + c):
            copy.start()
        return carry

    @pl.when(c == 0)
    def _():
        for copy in own_copies(0, 2 * z + 1):
            copy.start()

    lax.fori_loop(1, nz - z, begin, 0)

    def update(keys, values, gates, docs, causal, first):
        same = docs == col_ref[:, heads:heads + 1]
        if causal:
            qi = lax.broadcasted_iota(jnp.int32, (rows, rows), 0)
            ki = lax.broadcasted_iota(jnp.int32, (rows, rows), 1)
            same = same & (ki <= qi)
        for h in range(heads):
            scores = lax.dot_general(
                q_ref[h], keys, (((1,), (1,)), ((), ())), preferred_element_type=jnp.float32
            )
            scores = scores + col_ref[:, h:h + 1] - gates[h:h + 1, :]
            scores = jnp.where(same, scores, -jnp.inf)
            peak = jnp.max(scores, axis=-1, keepdims=True)
            if first:
                expo = jnp.exp(scores - peak)
                l_ref[h] = jnp.sum(expo, axis=-1, keepdims=True)
                m_ref[h] = peak
                acc_ref[h] = jnp.dot(
                    expo.astype(jnp.bfloat16), values, preferred_element_type=jnp.float32
                )
            else:
                old = m_ref[h]
                new = jnp.maximum(old, peak)
                expo = jnp.exp(scores - new)
                factor = jnp.exp(old - new)
                l_ref[h] = factor * l_ref[h] + jnp.sum(expo, axis=-1, keepdims=True)
                m_ref[h] = new
                acc_ref[h] = factor * acc_ref[h] + jnp.dot(
                    expo.astype(jnp.bfloat16), values, preferred_element_type=jnp.float32
                )

    update(
        kv_ref[:, :hd], kv_ref[:, hd:], gd_ref[...], gd_ref[heads:heads + 1, :], True, True
    )

    def take(source):
        update(
            kv_buf[source, :, :hd],
            kv_buf[source, :, hd:],
            gd_buf[source],
            gd_buf[source, heads:heads + 1, :],
            False,
            False,
        )

    def one_source(i, carry):
        dz = (i + 1) // 2
        direct = i % 2
        core = (1 - direct) * (1 - c) + direct * c
        source = 2 * (z - dz) + core
        for copy in fwd_copies(source, dz):
            copy.wait_recv()

        @pl.when(direct == 1)
        def _():
            for copy in fwd_copies(source, dz):
                copy.start()

        take(source)
        return carry

    lax.fori_loop(1 - c, 2 * z + 1, one_source, 0)

    for h in range(heads):
        att_ref[:, h * hd:(h + 1) * hd] = (acc_ref[h] / l_ref[h]).astype(jnp.bfloat16)

    share = rows // n_tp

    def project(i, carry):
        k = n_tp - 1 - i
        start = pl.multiple_of(flip(t, k) * share, share)
        block = jnp.dot(
            att_ref[pl.ds(start, share), :], w_ref[...], preferred_element_type=jnp.float32
        )
        sbuf[k] = block.astype(jnp.bfloat16)

        @pl.when(k > 0)
        def _():
            pltpu.make_async_remote_copy(
                sbuf.at[k], rbuf.at[k], rs_send.at[k], rs_recv.at[k],
                device_id={"tp": flip(t, k)}, device_id_type=MESH,
            ).start()

        return carry

    lax.fori_loop(0, n_tp, project, 0)

    for k in range(1, n_tp):
        copy = pltpu.make_async_remote_copy(
            sbuf.at[k], rbuf.at[k], rs_send.at[k], rs_recv.at[k],
            device_id={"tp": flip(t, k)}, device_id_type=MESH,
        )
        copy.wait_recv()

    def finish(i, carry):
        part = pl.ds(pl.multiple_of(i * CHUNK, CHUNK), CHUNK)
        total = sbuf[0, part, :].astype(jnp.float32)
        for k in range(1, n_tp):
            total = total + rbuf[k, part, :].astype(jnp.float32)
        mixed = (res_ref[part, :].astype(jnp.float32) + total).astype(jnp.bfloat16)
        mixed_ref[part, :] = mixed
        normed_ref[part, :] = rms_scale(mixed.astype(jnp.float32), gain_ref[...]).astype(
            jnp.bfloat16
        )
        return carry

    lax.fori_loop(0, share // CHUNK, finish, 0)

    for k in range(1, n_tp):
        pltpu.make_async_remote_copy(
            sbuf.at[k], rbuf.at[k], rs_send.at[k], rs_recv.at[k],
            device_id={"tp": flip(t, k)}, device_id_type=MESH,
        ).wait_send()

    def end(dz, carry):
        for copy in own_copies(dz, 2 * (z + dz) + c):
            copy.wait_send()
        return carry

    @pl.when(c == 0)
    def _():
        for copy in own_copies(0, 2 * z + 1):
            copy.wait_send()

    lax.fori_loop(1, nz - z, end, 0)

    def end_forward(dz, carry):
        for copy in fwd_copies(2 * (z - dz) + c, dz):
            copy.wait_send()
        return carry

    lax.fori_loop(1, z + 1, end_forward, 0)


def expert_kernel(
    nz,
    n_tp,
    out_ref,
    wg_hbm,
    wu_hbm,
    wd_hbm,
    ret_ref,
    wg_ref,
    wu_ref,
    wd_ref,
    arrived,
    part,
    pbuf,
    rbuf,
    hbuf,
    fin,
    w_sem,
    a_send,
    a_recv,
    b_send,
    b_recv,
    f_send,
    f_recv,
    d_send,
    d_recv,
    p_send,
    p_recv,
    h_send,
    h_recv,
    r_send,
    r_recv,
    z_send,
    z_recv,
):
    s = lax.axis_index("sp")
    t = lax.axis_index("tp")
    z, c = s // 2, s % 2
    _, cap, width = out_ref.shape
    rows = 2 * n_tp * cap
    partner = {"sp": 2 * z + 1 - c}
    near = 1 + c
    far = 2 - c

    loads = [
        pltpu.make_async_copy(src, dst, w_sem.at[i])
        for i, (src, dst) in enumerate(((wg_hbm, wg_ref), (wu_hbm, wu_ref), (wd_hbm, wd_ref)))
    ]
    for load in loads:
        load.start()
    greet(nz, n_tp, z, c, t)

    def remote(src, dst, send, recv, where):
        return pltpu.make_async_remote_copy(
            src, dst, send, recv, device_id=where, device_id_type=MESH
        )

    def source_of(q):
        return (z + nz - q) % nz

    def mine(q):
        return arrived.at[source_of(q), c, t]

    def along(q):
        target = (z + q) % nz
        return remote(
            out_ref.at[target], arrived.at[z, c, t], a_send.at[q], a_recv.at[q],
            {"sp": 2 * target + c},
        )

    def along_in(q):
        return remote(mine(q), mine(q), a_send.at[q], a_recv.at[q], partner)

    def spread(q, k, src):
        where = {"tp": flip(t, k)} if k else partner
        return remote(src, mine(q), b_send.at[k, q], b_recv.at[k, q], where)

    def spread_in(q, k):
        block = arrived.at[source_of(q), c, flip(t, k)] if k else arrived.at[
            source_of(q), 1 - c, t
        ]
        return remote(block, block, b_send.at[k, q], b_recv.at[k, q], partner)

    def diagonal(q):
        block = arrived.at[source_of(q), c, flip(t, far)]
        return remote(block, block, f_send.at[q], f_recv.at[q], {"tp": flip(t, near)})

    def diagonal_in(q):
        block = arrived.at[source_of(q), c, flip(t, 3)]
        return remote(block, block, f_send.at[q], f_recv.at[q], partner)

    def to_partner(q, k):
        block = arrived.at[source_of(q), c, flip(t, k)]
        return remote(block, block, d_send.at[k, q], d_recv.at[k, q], partner)

    def from_partner(q, k):
        block = arrived.at[source_of(q), 1 - c, flip(t, k)]
        return remote(block, block, d_send.at[k, q], d_recv.at[k, q], partner)

    def part_out(q):
        return remote(part.at[q, 1 - c], pbuf.at[q], p_send.at[q], p_recv.at[q], partner)

    def hand_over(q):
        return remote(
            part.at[q, c, flip(t, 3)], hbuf.at[q], h_send.at[q], h_recv.at[q],
            {"tp": flip(t, near)},
        )

    def reduce_near(q):
        return remote(
            part.at[q, c, flip(t, near)], rbuf.at[q, 0], r_send.at[0, q], r_recv.at[0, q],
            {"tp": flip(t, near)},
        )

    def reduce_far(q):
        return remote(
            part.at[q, c, flip(t, far)], rbuf.at[q, 1], r_send.at[1, q], r_recv.at[1, q],
            {"tp": flip(t, far)},
        )

    def home(q):
        return remote(
            fin.at[q], ret_ref.at[z], z_send.at[q], z_recv.at[q], {"sp": 2 * source_of(q) + c}
        )

    def home_in(q):
        return remote(
            fin.at[q], ret_ref.at[(z + q) % nz], z_send.at[q], z_recv.at[q], partner
        )

    for k in (1, 2, 0):
        spread(0, k, out_ref.at[z]).start()

    def begin(q, carry):
        along(q).start()
        return carry

    lax.fori_loop(1, nz, begin, 0)
    arrived[z, c, t] = out_ref[z]
    for load in loads:
        load.wait()

    def add_pair(q, column):
        def one(r, carry):
            at = pl.ds(pl.multiple_of(r * CHUNK, CHUNK), CHUNK)
            total = part[q, c, column, at, :].astype(jnp.float32) + pbuf[
                q, column, at, :
            ].astype(jnp.float32)
            part[q, c, column, at, :] = total.astype(jnp.bfloat16)
            return carry

        lax.fori_loop(0, cap // CHUNK, one, 0)

    def step(i, carry):
        p = i - 1

        @pl.when(p + 2 < nz)
        def _():
            q = p + 2
            along_in(q).wait_recv()
            for k in (1, 2, 0):
                spread(q, k, mine(q)).start()

        @pl.when(p + 1 < nz)
        def _():
            q = p + 1
            spread_in(q, 1).wait_recv()
            to_partner(q, 1).start()
            spread_in(q, 2).wait_recv()
            diagonal(q).start()
            to_partner(q, 2).start()
            spread_in(q, 0).wait_recv()

        @pl.when((p >= 0) & (p < nz))
        def _():
            diagonal_in(p).wait_recv()
            to_partner(p, 3).start()
            for k in range(1, n_tp):
                from_partner(p, k).wait_recv()
            flat = arrived[source_of(p)].reshape(rows, width)
            gate = jnp.dot(flat, wg_ref[...], preferred_element_type=jnp.float32)
            up = jnp.dot(flat, wu_ref[...], preferred_element_type=jnp.float32)
            hidden = (gate * (1.0 / (1.0 + jnp.exp(-gate))) * up).astype(jnp.bfloat16)
            result = jnp.dot(hidden, wd_ref[...], preferred_element_type=jnp.float32)
            part[p] = result.astype(jnp.bfloat16).reshape(2, n_tp, cap, width)
            part_out(p).start()

        @pl.when((p >= 1) & (p - 1 < nz))
        def _():
            q = p - 1
            part_out(q).wait_recv()
            add_pair(q, flip(t, 3))
            hand_over(q).start()
            add_pair(q, flip(t, near))
            reduce_near(q).start()
            add_pair(q, flip(t, far))
            add_pair(q, t)

        @pl.when((p >= 2) & (p - 2 < nz))
        def _():
            q = p - 2
            column = flip(t, far)
            hand_over(q).wait_recv()

            def one(r, carry):
                at = pl.ds(pl.multiple_of(r * CHUNK, CHUNK), CHUNK)
                total = part[q, c, column, at, :].astype(jnp.float32) + hbuf[q, at, :].astype(
                    jnp.float32
                )
                part[q, c, column, at, :] = total.astype(jnp.bfloat16)
                return carry

            lax.fori_loop(0, cap // CHUNK, one, 0)
            reduce_far(q).start()

        @pl.when(p >= 3)
        def _():
            q = p - 3
            reduce_near(q).wait_recv()
            reduce_far(q).wait_recv()

            def one(r, carry):
                at = pl.ds(pl.multiple_of(r * CHUNK, CHUNK), CHUNK)
                total = (
                    part[q, c, t, at, :].astype(jnp.float32)
                    + rbuf[q, 0, at, :].astype(jnp.float32)
                    + rbuf[q, 1, at, :].astype(jnp.float32)
                )
                fin[q, at, :] = total.astype(jnp.bfloat16)
                return carry

            lax.fori_loop(0, cap // CHUNK, one, 0)

            @pl.when(q > 0)
            def _():
                home(q).start()

            @pl.when(q == 0)
            def _():
                ret_ref[z] = fin[0]

        return carry

    lax.fori_loop(0, nz + 4, step, 0)

    def drain(q, carry):
        home_in(q).wait_recv()
        home(q).wait_send()
        along(q).wait_send()
        return carry

    lax.fori_loop(1, nz, drain, 0)

    def drain_plane(q, carry):
        for k in range(3):
            spread(q, k, mine(q)).wait_send()
        diagonal(q).wait_send()
        for k in range(1, n_tp):
            to_partner(q, k).wait_send()
        part_out(q).wait_send()
        hand_over(q).wait_send()
        reduce_near(q).wait_send()
        reduce_far(q).wait_send()
        return carry

    lax.fori_loop(0, nz, drain_plane, 0)


def local(
    nz,
    n_tp,
    queries,
    keys,
    values,
    log_gates,
    documents,
    query_gain,
    key_gain,
    out_weight,
    residual,
    norm_gain,
    routes,
    route_weights,
    w_gate,
    w_up,
    w_down,
):
    tok_dev, heads, head_size = queries.shape
    model_dim = residual.shape[1]
    rows_dev = tok_dev // n_tp
    n_sp = 2 * nz
    query_norm = (rms_scale(queries.astype(jnp.float32), query_gain) * head_size ** (-0.5)).astype(
        jnp.bfloat16
    )
    key_norm = rms_scale(keys[:, 0, :].astype(jnp.float32), key_gain).astype(jnp.bfloat16)
    kv = jnp.concatenate([key_norm, values[:, 0, :]], axis=1)
    pad = (-(heads + 1)) % 8
    gates_docs = jnp.concatenate(
        [
            log_gates,
            documents.astype(jnp.float32)[None, :],
            jnp.zeros((pad, tok_dev), jnp.float32),
        ],
        axis=0,
    )
    vmem = pl.BlockSpec(memory_space=pltpu.VMEM)
    hbm = pl.BlockSpec(memory_space=pl.ANY)
    dma = pltpu.SemaphoreType.DMA
    mixed, normed = pl.pallas_call(
        functools.partial(attend_kernel, nz, n_tp),
        out_shape=(
            jax.ShapeDtypeStruct((rows_dev, model_dim), jnp.bfloat16),
            jax.ShapeDtypeStruct((rows_dev, model_dim), jnp.bfloat16),
        ),
        in_specs=[vmem] * 7,
        out_specs=(vmem, vmem),
        scratch_shapes=[
            pltpu.VMEM((n_sp,) + kv.shape, jnp.bfloat16),
            pltpu.VMEM((n_sp,) + gates_docs.shape, jnp.float32),
            pltpu.VMEM((heads, tok_dev, 1), jnp.float32),
            pltpu.VMEM((heads, tok_dev, 1), jnp.float32),
            pltpu.VMEM((heads, tok_dev, head_size), jnp.float32),
            pltpu.VMEM((tok_dev, heads * head_size), jnp.bfloat16),
            pltpu.VMEM((n_tp, rows_dev, model_dim), jnp.bfloat16),
            pltpu.VMEM((n_tp, rows_dev, model_dim), jnp.bfloat16),
            dma((nz,)),
            dma((n_sp,)),
            dma((nz,)),
            dma((n_sp,)),
            dma((nz,)),
            dma((nz,)),
            dma((n_tp,)),
            dma((n_tp,)),
        ],
        compiler_params=pltpu.CompilerParams(
            collective_id=0, has_side_effects=True, vmem_limit_bytes=56 * 1024 * 1024
        ),
        name="attend",
    )(
        jnp.transpose(query_norm, (1, 0, 2)),
        kv,
        gates_docs,
        gates_docs.T,
        out_weight,
        residual,
        norm_gain[None, :],
    )

    experts = nz
    named = min(rows_dev, 6 * rows_dev // n_sp)
    capacity = named + (-named) % CHUNK
    expert_ids = jnp.arange(experts, dtype=jnp.int32)
    chosen = routes[:, :, None] == expert_ids[None, None, :]
    picked = jnp.sum(chosen.astype(jnp.float32), axis=1)
    weight_of = jnp.sum(jnp.where(chosen, route_weights[:, :, None], 0.0), axis=1)
    rank = jnp.cumsum(picked, axis=0) - 1.0
    slot_ids = jnp.arange(capacity).astype(jnp.float32)
    placing = picked.T[:, None, :] * (rank.T[:, None, :] == slot_ids[None, :, None]).astype(
        jnp.float32
    )
    outgoing = jnp.einsum(
        "ecr,rd->ecd", placing.astype(jnp.bfloat16), normed, preferred_element_type=jnp.float32
    ).astype(jnp.bfloat16)

    hidden_dev = w_gate.shape[2]
    block = (nz, capacity, model_dim)
    returned = pl.pallas_call(
        functools.partial(expert_kernel, nz, n_tp),
        out_shape=jax.ShapeDtypeStruct(block, jnp.bfloat16),
        in_specs=[vmem, hbm, hbm, hbm],
        out_specs=vmem,
        scratch_shapes=[
            pltpu.VMEM((model_dim, hidden_dev), jnp.bfloat16),
            pltpu.VMEM((model_dim, hidden_dev), jnp.bfloat16),
            pltpu.VMEM((hidden_dev, model_dim), jnp.bfloat16),
            pltpu.VMEM((nz, 2, n_tp) + block[1:], jnp.bfloat16),
            pltpu.VMEM((nz, 2, n_tp) + block[1:], jnp.bfloat16),
            pltpu.VMEM((nz, n_tp) + block[1:], jnp.bfloat16),
            pltpu.VMEM((nz, 2) + block[1:], jnp.bfloat16),
            pltpu.VMEM(block, jnp.bfloat16),
            pltpu.VMEM(block, jnp.bfloat16),
            dma((3,)),
            dma((nz,)),
            dma((nz,)),
            dma((3, nz)),
            dma((3, nz)),
            dma((nz,)),
            dma((nz,)),
            dma((n_tp, nz)),
            dma((n_tp, nz)),
            dma((nz,)),
            dma((nz,)),
            dma((nz,)),
            dma((nz,)),
            dma((2, nz)),
            dma((2, nz)),
            dma((nz,)),
            dma((nz,)),
        ],
        compiler_params=pltpu.CompilerParams(
            collective_id=1, has_side_effects=True, vmem_limit_bytes=60 * 1024 * 1024
        ),
        name="experts",
    )(outgoing, w_gate[0], w_up[0], w_down[0])

    combining = placing * weight_of.T[:, None, :]
    routed = jnp.einsum(
        "ecr,ecd->rd", combining, returned.astype(jnp.float32), precision=lax.Precision.HIGHEST
    )
    return (mixed.astype(jnp.float32) + routed).astype(jnp.bfloat16)


def solution(mesh):
    return jax.shard_map(
        functools.partial(local, mesh.shape["sp"] // 2, mesh.shape["tp"]),
        mesh=mesh,
        in_specs=(
            P(("grp", "sp"), "tp", None),
            P(("grp", "sp"), "tp", None),
            P(("grp", "sp"), "tp", None),
            P("tp", ("grp", "sp")),
            P(("grp", "sp")),
            P(),
            P(),
            P("tp", None),
            P(("grp", "sp", "tp"), None),
            P(),
            P(("grp", "sp", "tp"), None),
            P(("grp", "sp", "tp"), None),
            P("sp", None, "tp"),
            P("sp", None, "tp"),
            P("sp", "tp", None),
        ),
        out_specs=P(("grp", "sp", "tp"), None),
        check_vma=False,
    )
```
